32 devices in a mesh: sp: 4 (over z), fs: 4 (over y, x), tp: 2 (over core).
Axes of the slice: x: 2, y: 2, z: 4, core: 2. Of those that a mesh axis runs over, the one named last changes fastest.
Arguments:
- tokens: bfloat16 [8192, 2048], P(('fs', 'sp')), parts along dimension 0, may hold values from -6 to 6
- norm_gain: bfloat16 [2048], replicated, may hold values from 0.099609375 to 1.8984375
- w_query: bfloat16 [2048, 1024], P('sp', 'tp'), may hold values from -0.15625 to 0.15625
- w_key: bfloat16 [2048, 256], P('sp', 'tp'), may hold values from -0.15625 to 0.15625
- w_value: bfloat16 [2048, 256], P('sp', 'tp'), may hold values from -0.125 to 0.125
- w_glu_value: bfloat16 [2048, 1024], P('sp', 'tp'), may hold values from -0.22097087 to 0.22097087
- w_glu_gate: bfloat16 [2048, 1024], P('sp', 'tp'), may hold values from -0.125 to 0.125
- conv_taps: bfloat16 [31, 1024], P(None, 'tp'), may hold values from -1 to 1
- convolution_norm_gain: bfloat16 [1024], replicated, may hold values from 0.099609375 to 1.8984375
- head_gain: bfloat16 [128], replicated, may hold values from 0.099609375 to 1.8984375
- lam: float32 [8], P('tp'), may hold values from 0.3 to 0.8
- w_out: bfloat16 [2048, 2048], P(None, 'sp'), may hold values from -0.125 to 0.125
Outputs:
- mixed: bfloat16 [8192, 2048], P(('fs', 'sp', 'tp')), parts along dimension 0
- log_totals: float32 [8192, 16], P(('fs', 'sp'), 'tp'), parts along dimension 0
The draws below stay inside these ranges and needn't reach their ends.
There are 4 independent parts, one for each index of `fs`. The reference program is written for one: setup_inputs(seed, part) draws one part's arguments, and reference() takes and returns one part's arrays. A program takes and returns all parts, laid end to end along the dimension named above; an argument that names none is the same for every part. Nothing has to cross between parts.
All inputs are finite; a program needn't handle non-finite values.
Results may differ from the reference program's by a relative error of at most 0.0095.
Values may be sent and summed in bfloat16 or wider, within the bound.
No kernel may reach another device: no remote copies, remote signals or barrier semaphores. Data moves between devices by JAX's collectives and lax.ppermute only.
A program may use at most 64 MiB of HBM per device.

```python
import math
import jax
import jax.numpy as jnp
from jax import lax

D = 2048
HEADS = 8
KV_HEADS = 2
QK = 64
VDIM = 128
CONV = 1024
KW = 31
SEQ = 2048


def draw_w_glu_value(key, part):
    first, second = jax.random.split(jax.random.fold_in(key, 41))
    placed = (jnp.arange(CONV, dtype=jnp.float32) + jax.random.uniform(first, (CONV,), jnp.float32)) / CONV
    column_scale = 10.0 ** placed / 4.0
    base = jax.random.truncated_normal(second, -4.0, 4.0, (D, CONV), jnp.float32)
    values = base * column_scale[None, :] * D ** (-0.5)
    return jnp.clip(values, -10.0 * D ** (-0.5), 10.0 * D ** (-0.5)).astype(jnp.bfloat16)


def block_scale(own_key, dims, cuts, low, high):
    def one(axis_at, shards_of):
        draws = jax.random.uniform(jax.random.fold_in(jax.random.fold_in(own_key, 6), axis_at), (shards_of,), jnp.float32, low / len(cuts), high / len(cuts))
        return jnp.repeat(jnp.exp(draws), dims[axis_at] // shards_of).reshape((-1,) + (1,) * (len(dims) - axis_at - 1))

    level = one(*cuts[0])
    for cut in cuts[1:]:
        level = level * one(*cut)
    return level


def bell_draw(key, extent, scale, limit, cuts=(), kind=jnp.bfloat16):
    entries = jax.random.normal(key, extent, jnp.float32) * scale
    if len(cuts) > 0:
        entries = block_scale(key, extent, cuts, -0.22, 0.18) * entries
    return jnp.clip(entries, min=-limit, max=limit).astype(kind)


def setup_inputs(seed: int = 0, part: int = 0) -> dict:
    streams_of = jax.random.split(jax.random.key(seed), 13)
    part_keys = jax.random.split(jax.random.fold_in(streams_of[12], part), 13)
    return {
        "tokens": bell_draw(part_keys[0], (SEQ, D), 1.0, 6.0, ((0, 4),)),
        "norm_gain": jnp.clip(1.0 + 0.18 * jax.random.normal(streams_of[1], (D,), jnp.float32), 0.099609375, 1.8984375).astype(jnp.bfloat16),
        "w_query": bell_draw(streams_of[2], (D, HEADS * 2 * QK), (D * 2 // 3) ** -0.5, 0.15625, ((0, 4), (1, 2))),
        "w_key": bell_draw(streams_of[3], (D, KV_HEADS * 2 * QK), (D * 2 // 3) ** -0.5, 0.15625, ((0, 4), (1, 2))),
        "w_value": bell_draw(streams_of[4], (D, KV_HEADS * VDIM), D ** -0.5, 0.125, ((0, 4), (1, 2))),
        "w_glu_value": draw_w_glu_value(jax.random.fold_in(streams_of[12], 71), part),
        "w_glu_gate": bell_draw(streams_of[6], (D, CONV), D ** -0.5, 0.125, ((0, 4), (1, 2))),
        "conv_taps": bell_draw(streams_of[7], (KW, CONV), KW ** -0.5, 1.0, ((1, 2),)),
        "convolution_norm_gain": jnp.clip(1.0 + 0.18 * jax.random.normal(streams_of[8], (CONV,), jnp.float32), 0.099609375, 1.8984375).astype(jnp.bfloat16),
        "head_gain": jnp.clip(1.0 + 0.18 * jax.random.normal(streams_of[9], (VDIM,), jnp.float32), 0.099609375, 1.8984375).astype(jnp.bfloat16),
        "lam": jnp.clip(0.3 + 0.5 * jax.random.uniform(streams_of[10], (HEADS,), jnp.float32) ** block_scale(streams_of[10], (HEADS,), ((0, 2),), -0.2, 0.2), 0.3, 0.8),
        "w_out": bell_draw(streams_of[11], (HEADS * VDIM + CONV, D), (HEADS * VDIM + CONV) ** -0.5, 0.125, ((1, 4),)),
    }


def reference(tokens, norm_gain, w_query, w_key, w_value, w_glu_value, w_glu_gate, conv_taps, convolution_norm_gain, head_gain, lam, w_out):
    length = tokens.shape[0]
    eps = 1e-06
    tok32 = tokens.astype(jnp.float32)
    normalized_rows = (tok32 * lax.rsqrt(lax.optimization_barrier(jnp.mean(tok32 * tok32, axis=-1, keepdims=True)) + eps) * norm_gain.astype(jnp.float32)).astype(jnp.bfloat16)
    queries = jnp.dot(normalized_rows, w_query, preferred_element_type=jnp.float32).astype(jnp.bfloat16)
    keys = jnp.dot(normalized_rows, w_key, preferred_element_type=jnp.float32).astype(jnp.bfloat16)
    values = jnp.dot(normalized_rows, w_value, preferred_element_type=jnp.float32).astype(jnp.bfloat16)
    glu_val = jnp.dot(normalized_rows, w_glu_value, preferred_element_type=jnp.float32)
    glu_gate = jnp.dot(normalized_rows, w_glu_gate, preferred_element_type=jnp.float32)
    gated = (glu_val * jax.nn.sigmoid(glu_gate)).astype(jnp.bfloat16)
    padded = jnp.concatenate([jnp.zeros((KW - 1, CONV), jnp.bfloat16), gated], axis=0)
    conv = jnp.zeros((length, CONV), jnp.float32)
    for tap in range(KW):
        conv = conv + conv_taps[tap].astype(jnp.float32) * padded[tap:tap + length].astype(jnp.float32)
    conv = conv.astype(jnp.bfloat16).astype(jnp.float32)
    conv_act = jax.nn.silu(conv * lax.rsqrt(lax.optimization_barrier(jnp.mean(conv * conv, axis=-1, keepdims=True)) + eps) * convolution_norm_gain.astype(jnp.float32)).astype(jnp.bfloat16)
    group = HEADS // KV_HEADS
    key_all = keys.astype(jnp.float32).reshape(length, KV_HEADS, 2, QK)
    value_rows_full = values.astype(jnp.float32).reshape(length, KV_HEADS, VDIM)
    block = math.gcd(length, 512)
    query_blocks = queries.reshape(length // block, block, KV_HEADS, group, 2, QK)
    key_pos = jnp.arange(length, dtype=jnp.int32)

    def one_block(item):
        query_block, index = item
        qfloat = query_block.astype(jnp.float32)
        score = jnp.einsum('tkgmd,nkmd->tkgmn', qfloat, key_all) * QK ** (-0.5)
        query_pos = index * block + jnp.arange(block, dtype=jnp.int32)
        allowed = key_pos[None, None, None, None, :] <= query_pos[:, None, None, None, None]
        weight = jnp.where(allowed, jnp.exp(score), 0.0)
        total = lax.optimization_barrier(jnp.sum(weight, axis=-1))
        rounded_values = weight.astype(jnp.bfloat16).astype(jnp.float32)
        running_total = jnp.einsum('doejz,zow->doejw', rounded_values, value_rows_full)
        return (running_total, total)
    running_total, total = lax.map(one_block, (query_blocks, jnp.arange(length // block, dtype=jnp.int32)))
    running_total = running_total.reshape(length, HEADS, 2, VDIM)
    total = total.reshape(length, HEADS, 2)
    lam32 = lam.astype(jnp.float32)
    diff = running_total[:, :, 0] / total[:, :, 0, None] - lam32[None, :, None] * running_total[:, :, 1] / total[:, :, 1, None]
    att_out = diff * lax.rsqrt(lax.optimization_barrier(jnp.mean(diff * diff, axis=-1, keepdims=True)) + eps) * head_gain.astype(jnp.float32)
    att_out = att_out.astype(jnp.bfloat16).reshape(length, HEADS * VDIM)
    log_totals = jnp.log(total).reshape(length, HEADS * 2)
    both = jnp.concatenate([att_out, conv_act], axis=1)
    mixed = jnp.dot(both, w_out, preferred_element_type=jnp.float32).astype(jnp.bfloat16)
    return (mixed, log_totals)
```

```python
import functools
import math

import jax
import jax.numpy as jnp
from jax import lax
from jax.experimental import pallas as pl
from jax.experimental.pallas import tpu as pltpu
from jax.sharding import PartitionSpec as P

QK = 64
VDIM = 128
EPS = 1e-06
F32 = jnp.float32
BF16 = jnp.bfloat16
VMEM = pl.BlockSpec(memory_space=pltpu.VMEM)
SMEM = pl.BlockSpec(memory_space=pltpu.SMEM)


PAIRS_X = [(0, 1), (1, 0), (2, 3), (3, 2)]
PAIRS_Y = [(0, 2), (2, 0), (1, 3), (3, 1)]
LINE_1 = [(0, 1), (1, 0), (2, 3), (3, 2)]
LINE_2 = [(1, 2), (2, 1)]
LINE_3 = [(1, 0), (2, 3)]


def call(kernel, outs, args, specs, scratch=(), flops=0, bytes_accessed=0, name=None):
    return pl.pallas_call(
        kernel,
        out_shape=outs,
        in_specs=specs,
        out_specs=jax.tree.map(lambda _: VMEM, outs),
        scratch_shapes=list(scratch),
        compiler_params=pltpu.CompilerParams(vmem_limit_bytes=48 * 1024 * 1024),
        cost_estimate=pl.CostEstimate(
            flops=int(flops), bytes_accessed=int(bytes_accessed), transcendentals=0
        ),
        name=name,
    )(*args)


def norm_kernel(tok_ref, gain_ref, out_ref):
    rows = tok_ref.shape[0]
    step = math.gcd(rows, 64)
    gain = gain_ref[...].astype(F32)

    @pl.loop(0, rows // step)
    def _(r):
        at = pl.ds(pl.multiple_of(r * step, step), step)
        x = tok_ref[at, :].astype(F32)
        scale = lax.rsqrt(jnp.mean(x * x, axis=-1, keepdims=True) + EPS)
        out_ref[at, :] = (x * scale * gain).astype(BF16)


def place(piece, pos_ref, per_shard):
    kind, k = piece
    if kind == "abs":
        return k // per_shard, k % per_shard
    me, c = pos_ref[0], pos_ref[1]
    if kind == "near":
        shard = me + 1 - 2 * (me % 2)
    elif kind == "far0":
        shard = jnp.where(me < 2, 2, 1)
    else:
        shard = jnp.where(me < 2, 3, 0)
    return shard, lax.bitwise_xor(c, jnp.int32(k))


def assemble(pos_ref, own_refs, piece_refs, pieces, full_ref, piece_rows):
    own_rows = own_refs[0].shape[0]
    col = 0
    at = pl.ds(pl.multiple_of(pos_ref[0] * own_rows, own_rows), own_rows)
    for ref in own_refs:
        full_ref[at, col : col + ref.shape[1]] = ref[...]
        col += ref.shape[1]
    k = 0
    for ref in piece_refs:
        for j in range(ref.shape[0] // piece_rows):
            shard, part = place(pieces[k], pos_ref, own_rows // piece_rows)
            start = shard * own_rows + part * piece_rows
            if not isinstance(start, int):
                start = pl.multiple_of(start, piece_rows)
            full_ref[pl.ds(start, piece_rows), :] = ref[j * piece_rows : (j + 1) * piece_rows, :]
            k += 1


def qkv_kernel(piece_rows, pieces, n_refs, pos_ref, x_ref, wk_ref, wv_ref, wq_ref, *rest):
    piece_refs, (kv_ref, q_ref, full_ref) = rest[:n_refs], rest[n_refs:]
    assemble(pos_ref, (wk_ref, wv_ref, wq_ref), piece_refs, pieces, full_ref, piece_rows)
    kv_cols = wk_ref.shape[1] + wv_ref.shape[1]
    x = x_ref[...]
    kv_ref[...] = jnp.dot(x, full_ref[:, :kv_cols], preferred_element_type=F32).astype(BF16)
    width = math.gcd(q_ref.shape[1], 256)
    for c in range(0, q_ref.shape[1], width):
        q_ref[:, c : c + width] = jnp.dot(
            x, full_ref[:, kv_cols + c : kv_cols + c + width], preferred_element_type=F32
        ).astype(BF16)


def glu_kernel(piece_rows, pieces, n_refs, pos_ref, x_ref, wa_ref, wb_ref, *rest):
    piece_refs, (out_ref, full_ref) = rest[:n_refs], rest[n_refs:]
    assemble(pos_ref, (wa_ref, wb_ref), piece_refs, pieces, full_ref, piece_rows)
    cols = out_ref.shape[1]
    x = x_ref[...]
    width = math.gcd(cols, 256)
    for c in range(0, cols, width):
        value = jnp.dot(x, full_ref[:, c : c + width], preferred_element_type=F32)
        gate = jnp.dot(x, full_ref[:, cols + c : cols + c + width], preferred_element_type=F32)
        out_ref[:, c : c + width] = (value * jax.nn.sigmoid(gate)).astype(BF16)


def conv_kernel(halo_ref, gated_ref, taps_ref, out_ref, sq_ref, pad_ref, sum_ref):
    rows, cols = gated_ref.shape
    taps = taps_ref.shape[0]
    head = halo_ref.shape[0]
    pad_ref[0:head, :] = halo_ref[...].astype(F32)
    pad_ref[head : head + rows, :] = gated_ref[...].astype(F32)
    first = head - (taps - 1)
    tile = math.gcd(rows, 64)
    sum_ref[...] = jnp.zeros_like(sum_ref)

    @pl.loop(0, cols // 128)
    def _(c):
        lanes = pl.ds(pl.multiple_of(c * 128, 128), 128)
        for r in range(0, rows, tile):
            acc = jnp.zeros((tile, 128), F32)
            for j in range(taps):
                acc = acc + taps_ref[j : j + 1, lanes].astype(F32) * pad_ref[
                    r + first + j : r + first + j + tile, lanes
                ]
            rounded = acc.astype(BF16)
            out_ref[r : r + tile, lanes] = rounded
            wide = rounded.astype(F32)
            sum_ref[r : r + tile, :] += wide * wide

    sq_ref[...] = jnp.broadcast_to(
        jnp.sum(sum_ref[...], axis=-1, keepdims=True), sq_ref.shape
    )


def attention_kernel(group, behind, pos_ref, lam_ref, q_ref, gain_ref, own_ref, *rest):
    kv_refs, (out_ref, log_ref, acc_ref, vext_ref, qs_ref) = rest[: len(behind)], rest[len(behind) :]
    rows = q_ref.shape[0]
    me = pos_ref[0]
    scale = QK ** (-0.5) * math.log2(math.e)
    for h in range(group):
        for m in range(2):
            c = (h * 2 + m) * QK
            qs_ref[m, h * rows : (h + 1) * rows, :] = q_ref[:, c : c + QK]
    vext_ref[:, VDIM:] = jnp.ones((rows, VDIM), BF16)
    tile = math.gcd(rows, 256)

    def weigh(m, at, keys):
        score = lax.dot_general(
            qs_ref[m, at, :], keys, (((1,), (1,)), ((), ())), preferred_element_type=F32
        )
        return jnp.exp2(score * scale)

    def add(weight, vals):
        return jnp.dot(weight.astype(BF16), vals, preferred_element_type=F32)

    vext_ref[:, :VDIM] = own_ref[:, 2 * QK :]
    for m in range(2):

        @pl.loop(0, group)
        def _(h):
            for r in range(rows // tile):
                at = pl.ds(pl.multiple_of(h * rows + r * tile, tile), tile)
                keys = (r + 1) * tile
                weight = weigh(m, at, own_ref[:keys, m * QK : (m + 1) * QK])
                t = r * tile + lax.broadcasted_iota(jnp.int32, weight.shape, 0)
                s = lax.broadcasted_iota(jnp.int32, weight.shape, 1)
                weight = jnp.where(s <= t, weight, 0.0)
                acc_ref[m, at, :] = add(weight, vext_ref[:keys, :])

    def earlier(ref, start):
        at_keys = pl.ds(start, rows)
        vext_ref[:, :VDIM] = ref[at_keys, 2 * QK :]
        for m in range(2):
            keys = ref[at_keys, m * QK : (m + 1) * QK]

            @pl.loop(0, group)
            def _(h):
                for r in range(rows // tile):
                    at = pl.ds(pl.multiple_of(h * rows + r * tile, tile), tile)
                    acc_ref[m, at, :] += add(weigh(m, at, keys), vext_ref[...])

    for ref, least in zip(kv_refs, behind):
        if len(least) == 1:
            pl.when(me >= least[0])(functools.partial(earlier, ref, 0))
        else:

            @pl.loop(0, len(least))
            def _(b):
                @pl.when(me >= b + least[0])
                def _():
                    earlier(ref, pl.multiple_of(b * rows, rows))

    gain = gain_ref[...].astype(F32)
    logs = []
    for h in range(group):
        at = slice(h * rows, (h + 1) * rows)
        total0 = acc_ref[0, at, VDIM:]
        total1 = acc_ref[1, at, VDIM:]
        diff = acc_ref[0, at, :VDIM] / total0 - lam_ref[h] * acc_ref[1, at, :VDIM] / total1
        scale_h = lax.rsqrt(jnp.mean(diff * diff, axis=-1, keepdims=True) + EPS)
        out_ref[:, h * VDIM : (h + 1) * VDIM] = (diff * scale_h * gain).astype(BF16)
        logs.append(total0[:, :1])
        logs.append(total1[:, :1])
    log_ref[...] = jnp.log(jnp.concatenate(logs, axis=1))


def out_kernel(
    pieces, n_refs, piece_rows, all_channels, mine, pos_ref, att_ref, conv_ref, sq_ref,
    sq2_ref, gain_ref, own_a_ref, own_c_ref, *rest
):
    piece_refs, rest = rest[:n_refs], rest[n_refs:]
    out_ref, full_ref = rest[-2:]
    half = out_ref.shape[0]
    cols = own_a_ref.shape[1]
    att_cols, channels = att_ref.shape[1], conv_ref.shape[1]
    own = pl.ds(pl.multiple_of(pos_ref[0] * cols, cols), cols)
    full_ref[:att_cols, own] = own_a_ref[...]
    full_ref[att_cols:, own] = own_c_ref[...]
    k = 0
    for ref in piece_refs:
        for j in range(ref.shape[0] // piece_rows):
            shard, part = place(pieces[k], pos_ref, full_ref.shape[0] // piece_rows)
            row, col = part * piece_rows, shard * cols
            if not isinstance(row, int):
                row, col = pl.multiple_of(row, piece_rows), pl.multiple_of(col, cols)
            full_ref[pl.ds(row, piece_rows), pl.ds(col, cols)] = ref[
                j * piece_rows : (j + 1) * piece_rows, :
            ]
            k += 1
    t = pos_ref[2]
    take = pl.ds(pl.multiple_of((t if mine else 1 - t) * half, half), half)
    total = sq_ref[take, :1] + sq2_ref[take, :1]
    conv = conv_ref[take, :].astype(F32)
    pre = conv * lax.rsqrt(total / all_channels + EPS) * gain_ref[...].astype(F32)
    act = (pre * jax.nn.sigmoid(pre)).astype(BF16)
    both = jnp.concatenate([att_ref[take, :], act], axis=1)
    width = math.gcd(out_ref.shape[1], 512)
    for c in range(0, out_ref.shape[1], width):
        part = jnp.dot(both, full_ref[:, c : c + width], preferred_element_type=F32)
        if mine:
            part = part + rest[0][:, c : c + width].astype(F32)
        out_ref[:, c : c + width] = part.astype(BF16)


def shift(array, axis, pairs):
    return lax.ppermute(array, axis, pairs)


def gather_line(mid, near_own):
    near = shift(near_own, "sp", LINE_1)
    second = shift(jnp.concatenate([near_own, near], axis=0), "sp", LINE_2)
    third = shift(second, "sp", LINE_3)
    return near, jnp.where(mid, second, third)


def gather_near(array, first, second, k1, k2):
    got = shift(array, "fs", first)
    rest = shift(jnp.concatenate([array, got], axis=0), "fs", second)
    return [array, got, rest], [("near", 0), ("near", k1), ("near", k2), ("near", k1 ^ k2)]


def gather_far(array):
    half = array.shape[0] // 2
    by_x = shift(array, "fs", PAIRS_X)
    by_y = shift(array, "fs", PAIRS_Y)
    on_x = shift(by_y[:half], "fs", PAIRS_X)
    on_y = shift(by_x[half:], "fs", PAIRS_Y)
    kinds = [("far0", 0), ("far1", 0), ("far0", 1), ("far1", 1), ("far0", 2), ("far1", 2)]
    return [array, by_x, by_y, on_x, on_y], kinds + [("far0", 3), ("far1", 3)]


def gather_weight(planes, mid, own, quarter, order):
    if not planes:
        whole = lax.all_gather(own(), "sp", axis=0, tiled=True)
        return [whole], None
    near, far = gather_line(mid, quarter())
    ways = (PAIRS_X, PAIRS_Y, 1, 2) if order else (PAIRS_Y, PAIRS_X, 2, 1)
    a1, p1 = gather_near(near, *ways)
    a2, p2 = gather_far(far)
    return a1 + a2, tuple(p1 + p2)


def body(
    planes,
    tokens,
    norm_gain,
    w_query,
    w_key,
    w_value,
    w_glu_value,
    w_glu_gate,
    conv_taps,
    convolution_norm_gain,
    head_gain,
    lam,
    w_out,
):
    rows, width = tokens.shape
    me = lax.axis_index("sp")
    c = lax.axis_index("fs")
    t = lax.axis_index("tp")
    peers = lax.axis_size("sp")
    pos = jnp.stack([me, c, t]).astype(jnp.int32)
    mid = jnp.logical_or(me == 1, me == 2)

    own_rows = w_query.shape[0]
    parts = 4 if planes else 1
    piece_rows = own_rows // parts
    heads_here = lam.shape[0]
    att_cols, channels = heads_here * VDIM, conv_taps.shape[1]
    all_att = w_out.shape[0] - convolution_norm_gain.shape[0]
    own_att = lax.dynamic_slice_in_dim(w_out, t * att_cols, att_cols, 0)
    own_conv = lax.dynamic_slice_in_dim(w_out, all_att + t * channels, channels, 0)
    out_rows = (att_cols + channels) // parts

    def quarter(arrays):
        return lambda: jnp.concatenate(
            [lax.dynamic_slice_in_dim(a, c * piece_rows, piece_rows, 0) for a in arrays], axis=1
        )

    def out_quarter():
        start = jnp.where(
            c < 2, t * att_cols + c * out_rows, all_att + t * channels + (c - 2) * out_rows
        )
        return lax.dynamic_slice_in_dim(w_out, start, out_rows, 0)

    in_a = (w_key, w_value, w_query)
    in_b = (w_glu_value, w_glu_gate)
    qkv_arrays, qkv_pieces = gather_weight(
        planes, mid, lambda: jnp.concatenate(in_a, axis=1), quarter(in_a), True
    )
    glu_arrays, glu_pieces = gather_weight(
        planes, mid, lambda: jnp.concatenate(in_b, axis=1), quarter(in_b), False
    )
    out_arrays, out_pieces = gather_weight(
        planes, mid, lambda: jnp.concatenate([own_att, own_conv], axis=0), out_quarter, True
    )
    if not planes:
        qkv_pieces = glu_pieces = out_pieces = tuple(("abs", k) for k in range(peers))

    normed = call(
        norm_kernel,
        jax.ShapeDtypeStruct((rows, width), BF16),
        (tokens, norm_gain[None, :]),
        [VMEM, VMEM],
        flops=rows * width * 4,
        bytes_accessed=rows * width * 4,
        name="norm",
    )

    kv_cols = w_key.shape[1] + w_value.shape[1]
    q_cols = w_query.shape[1]
    kv, queries = call(
        functools.partial(qkv_kernel, piece_rows, qkv_pieces, len(qkv_arrays)),
        [
            jax.ShapeDtypeStruct((rows, kv_cols), BF16),
            jax.ShapeDtypeStruct((rows, q_cols), BF16),
        ],
        (pos, normed, *in_a, *qkv_arrays),
        [SMEM] + [VMEM] * (4 + len(qkv_arrays)),
        scratch=[pltpu.VMEM((width, kv_cols + q_cols), BF16)],
        flops=2 * rows * width * (kv_cols + q_cols),
        bytes_accessed=2 * width * (kv_cols + q_cols + rows),
        name="qkv",
    )
    if planes:
        one = shift(kv, "sp", [(k, k + 1) for k in range(peers - 1)])
        two = shift(one, "sp", [(k, k + 1) for k in range(1, peers - 1)])
        three = shift(two, "sp", [(k, k + 1) for k in range(2, peers - 1)])
        earlier, behind = [one, two, three], ((1,), (2,), (3,))
    else:
        earlier = [lax.all_gather(kv, "sp", axis=0, tiled=True)]
        behind = (tuple(range(1, peers + 1)),)

    gated = call(
        functools.partial(glu_kernel, piece_rows, glu_pieces, len(glu_arrays)),
        jax.ShapeDtypeStruct((rows, channels), BF16),
        (pos, normed, *in_b, *glu_arrays),
        [SMEM] + [VMEM] * (3 + len(glu_arrays)),
        scratch=[pltpu.VMEM((width, 2 * channels), BF16)],
        flops=4 * rows * width * channels,
        bytes_accessed=2 * width * (2 * channels + rows),
        name="glu",
    )
    taps = conv_taps.shape[0]
    head = (taps - 1 + 15) // 16 * 16
    halo = shift(gated[rows - head :], "sp", [(k, k + 1) for k in range(peers - 1)])
    conv, squares = call(
        conv_kernel,
        [
            jax.ShapeDtypeStruct((rows, channels), BF16),
            jax.ShapeDtypeStruct((rows, 128), F32),
        ],
        (halo, gated, conv_taps),
        [VMEM] * 3,
        scratch=[pltpu.VMEM((head + rows, channels), F32), pltpu.VMEM((rows, 128), F32)],
        flops=400 * rows * taps * channels,
        bytes_accessed=4 * rows * channels,
        name="conv",
    )
    swap = [(0, 1), (1, 0)]
    squares2 = shift(squares, "tp", swap)

    kv_here = w_key.shape[1] // (2 * QK)
    group = heads_here // kv_here
    att_out, log_totals = call(
        functools.partial(attention_kernel, group, behind),
        [
            jax.ShapeDtypeStruct((rows, att_cols), BF16),
            jax.ShapeDtypeStruct((rows, heads_here * 2), F32),
        ],
        (pos, lam, queries, head_gain[None, :], kv, *earlier),
        [SMEM, SMEM] + [VMEM] * (3 + len(earlier)),
        scratch=[
            pltpu.VMEM((2, group * rows, 2 * VDIM), F32),
            pltpu.VMEM((rows, 2 * VDIM), BF16),
            pltpu.VMEM((2, group * rows, QK), BF16),
        ],
        flops=10e9,
        bytes_accessed=8 * rows * att_cols,
        name="attention",
    )

    gain_here = lax.dynamic_slice_in_dim(convolution_norm_gain, t * channels, channels, 0)[None, :]
    half = rows // 2
    out_cols = w_out.shape[1] * peers

    def project(mine, *more):
        return call(
            functools.partial(
                out_kernel,
                out_pieces,
                len(out_arrays),
                out_rows,
                convolution_norm_gain.shape[0],
                mine,
            ),
            jax.ShapeDtypeStruct((half, out_cols), BF16),
            (pos, att_out, conv, squares, squares2, gain_here, own_att, own_conv)
            + (*out_arrays, *more),
            [SMEM] + [VMEM] * (7 + len(out_arrays) + len(more)),
            scratch=[pltpu.VMEM((att_cols + channels, out_cols), BF16)],
            flops=2 * half * (att_cols + channels) * out_cols,
            bytes_accessed=2 * out_cols * (att_cols + channels + half),
            name="project",
        )

    given = shift(project(False), "tp", swap)
    mixed = project(True, given)
    return (mixed, log_totals)


def solution(mesh):
    planes = mesh.shape["sp"] == 4 and mesh.shape["fs"] == 4
    return jax.shard_map(
        functools.partial(body, planes),
        mesh=mesh,
        in_specs=(
            P(("fs", "sp"), None),
            P(),
            P("sp", "tp"),
            P("sp", "tp"),
            P("sp", "tp"),
            P("sp", "tp"),
            P("sp", "tp"),
            P(None, "tp"),
            P(),
            P(),
            P("tp"),
            P(None, "sp"),
        ),
        out_specs=(P(("fs", "sp", "tp"), None), P(("fs", "sp"), "tp")),
        check_vma=False,
    )
```
